32 devices in a mesh: sp: 8 (over z, y), tp: 4 (over x, core).
Axes of the slice: x: 2, y: 2, z: 4, core: 2. Of those that a mesh axis runs over, the one named last changes fastest.
Arguments:
- residual: bfloat16 [6144, 2048], P(('sp', 'tp')), may hold values from -6 to 6
- queries: bfloat16 [6144, 1024], P('sp', 'tp'), may hold values from -240 to 240
- keys: bfloat16 [6144, 256], P('sp', 'tp'), may hold values from -6 to 6
- values: bfloat16 [6144, 256], P('sp', 'tp'), may hold values from -18 to 18
- sinks: float32 [16], P('tp'), may hold values from 1 to 6
- out_weight: bfloat16 [1024, 2048], replicated, may hold values from -0.5625 to 0.5625
- norm_gain: float32 [2048], replicated, may hold values from 0.1 to 1.9
- gate_weight: bfloat16 [2048, 5632], P('sp', 'tp'), may hold values from -0.125 to 0.125
- up_weight: bfloat16 [2048, 5632], P('sp', 'tp'), may hold values from -0.125 to 0.125
- down_weight: bfloat16 [5632, 2048], P('tp', 'sp'), may hold values from -0.078125 to 0.078125
Outputs:
- layer_out: bfloat16 [6144, 2048], P(('sp', 'tp'))
The draws below stay inside these ranges and needn't reach their ends.
All inputs are finite; a program needn't handle non-finite values.
Results may differ from the reference program's by a relative error of at most 0.014.
Values may be sent and summed in bfloat16 or wider, within the bound.
No kernel may reach another device: no remote copies, remote signals or barrier semaphores. Data moves between devices by JAX's collectives and lax.ppermute only.
A program may use at most 128 MiB of HBM per device.

```python
import jax
import jax.numpy as jnp
from jax import lax

D = 2048
FF = 5632
HEAD = 64
QH = 16
KVH = 4
WINDOW = 128
ATT = 1024
TOKENS = 6144
N_TP = 4


def drawn(key):
    key_query, key_keys = jax.random.split(jax.random.fold_in(key, 7), 2)
    queries = jnp.clip(jax.random.normal(key_query, (TOKENS, QH * HEAD), jnp.float32), -6.0, 6.0)
    keyset = jnp.clip(jax.random.normal(key_keys, (TOKENS, KVH * HEAD), jnp.float32), -6.0, 6.0)
    return (queries, keyset)


def draw_queries(key, part):
    return drawn(key)[0].astype(jnp.bfloat16)


def draw_keys(key, part):
    return drawn(key)[1].astype(jnp.bfloat16)


def steps_of(rng, extent, shards, least, largest):
    def one(axis_at, shards_of):
        draws = jax.random.uniform(jax.random.fold_in(jax.random.fold_in(rng, 6), axis_at), (shards_of,), jnp.float32, least / len(shards), largest / len(shards))
        return jnp.repeat(jnp.exp(draws), extent[axis_at] // shards_of).reshape((-1,) + (1,) * (len(extent) - axis_at - 1))

    loudness = one(*shards[0])
    for cut in shards[1:]:
        loudness = loudness * one(*cut)
    return loudness


def gaussian(own_key, extent, spread, bound, shards=(), dtype=jnp.bfloat16):
    values = spread * jax.random.normal(own_key, extent, jnp.float32)
    if shards:
        values = values * steps_of(own_key, extent, shards, -0.22, 0.18)
    return jnp.clip(values, -bound, bound).astype(dtype)


def setup_inputs(seed: int = 0) -> dict:
    splits = jax.random.split(jax.random.key(seed), 11)
    residual = gaussian(splits[0], (TOKENS, D), 1.0, 6.0, ((0, 32),))
    queries = draw_queries(jax.random.fold_in(splits[10], 71), 0)
    keys = draw_keys(jax.random.fold_in(splits[10], 71), 0)
    values = gaussian(splits[3], (TOKENS, KVH * HEAD), 3.0, 18.0, ((0, 8), (1, 4)))
    sinks = jnp.clip(1.0 + 5.0 * jax.random.uniform(splits[4], (QH,), jnp.float32) ** steps_of(splits[4], (QH,), ((0, 4),), -0.2, 0.2), 1.0, 6.0)
    out_weight = gaussian(splits[5], (ATT, D), (3.0 / ATT ** 0.5), 0.5625)
    norm_gain = jnp.clip(1.0 + 0.18 * jax.random.normal(splits[6], (D,), jnp.float32), 0.1, 1.9)
    gate_weight = gaussian(splits[7], (D, FF), D ** -0.5, 0.125, ((0, 8), (1, 4)))
    up_weight = gaussian(splits[8], (D, FF), D ** -0.5, 0.125, ((0, 8), (1, 4)))
    down_weight = gaussian(splits[9], (FF, D), FF ** -0.5, 0.078125, ((0, 4), (1, 8)))
    return {"residual": residual, "queries": queries, "keys": keys, "values": values, "sinks": sinks, "out_weight": out_weight, "norm_gain": norm_gain, "gate_weight": gate_weight, "up_weight": up_weight, "down_weight": down_weight}


def attend(queries, keys_ext, values_ext, sinks, block_base):
    rows = queries.shape[0]
    nblk = rows // WINDOW
    qheads = sinks.shape[0]
    kheads = keys_ext.shape[1] // HEAD
    group = qheads // kheads
    qblock = queries.reshape(nblk, WINDOW, kheads, group, HEAD).astype(jnp.float32)

    def band(arr):
        first = arr[:rows].reshape(nblk, WINDOW, kheads, HEAD)
        second = arr[WINDOW:].reshape(nblk, WINDOW, kheads, HEAD)
        return jnp.concatenate([first, second], axis=1).astype(jnp.float32)
    kband = band(keys_ext)
    vband = band(values_ext)
    score = jnp.einsum('nqhgd,nkhd->nhgqk', qblock, kband) * HEAD ** (-0.5)
    qidx = jnp.arange(WINDOW)[:, None]
    kidx = jnp.arange(2 * WINDOW)[None, :]
    rel = qidx + WINDOW - kidx
    valid = (rel >= 0) & (rel < WINDOW)
    blocks = block_base + jnp.arange(nblk)
    valid = valid[None] & ((blocks > 0)[:, None, None] | (kidx >= WINDOW)[None])
    score = jnp.where(valid[:, None, None], score, -jnp.inf)
    sink = sinks.astype(jnp.float32).reshape(kheads, group)[None, :, :, None]
    top = jnp.maximum(lax.optimization_barrier(jnp.max(score, axis=-1)), sink)
    expd = jnp.exp(score - top[..., None])
    denom = lax.optimization_barrier(jnp.sum(expd, axis=-1)) + jnp.exp(sink - top)
    weights = (expd / denom[..., None]).astype(jnp.bfloat16)
    result = jnp.einsum('nhgqk,nkhd->nqhgd', weights.astype(jnp.float32), vband)
    return result.reshape(rows, qheads * HEAD).astype(jnp.bfloat16)

def reference(residual, queries, keys, values, sinks, out_weight, norm_gain, gate_weight, up_weight, down_weight):
    padding = jnp.zeros((WINDOW, keys.shape[1]), jnp.bfloat16)
    keys_ext = jnp.concatenate([padding, keys], axis=0)
    values_ext = jnp.concatenate([padding, values], axis=0)
    attention = attend(queries, keys_ext, values_ext, sinks, 0)
    proj = jnp.dot(attention, out_weight, preferred_element_type=jnp.float32)
    mixed = (residual.astype(jnp.float32) + proj).astype(jnp.bfloat16)
    mixf = mixed.astype(jnp.float32)
    normed = (mixf * lax.rsqrt(lax.optimization_barrier(jnp.mean(mixf * mixf, axis=-1, keepdims=True)) + 1e-06) * norm_gain).astype(jnp.bfloat16)
    gate = jnp.dot(normed, gate_weight, preferred_element_type=jnp.float32)
    upper = jnp.dot(normed, up_weight, preferred_element_type=jnp.float32)
    hidden = (jax.nn.silu(gate) * upper).astype(jnp.bfloat16)
    share = FF // N_TP
    ffn = jnp.zeros((hidden.shape[0], D), jnp.float32)
    for index in range(N_TP):
        part_sum = jnp.dot(hidden[:, index * share:(index + 1) * share], down_weight[index * share:(index + 1) * share], preferred_element_type=jnp.float32)
        ffn = ffn + lax.optimization_barrier(part_sum.astype(jnp.bfloat16)).astype(jnp.float32)
    return (mixed.astype(jnp.float32) + ffn).astype(jnp.bfloat16)
```

```python
import jax
import jax.numpy as jnp
from jax import lax
from jax.sharding import PartitionSpec as P


HEAD = 64
WINDOW = 128
LANES = 128


def passed_along(block, axis, distance):
    devices = range(lax.axis_size(axis))
    route = [(i - distance, i) for i in devices if i - distance in devices]
    return lax.ppermute(block, axis, route)


def attend(queries, keys_ext, values_ext, sinks, block_base):
    rows = queries.shape[0]
    nblk = rows // WINDOW
    qheads = sinks.shape[0]
    kheads = keys_ext.shape[1] // HEAD
    group = qheads // kheads
    qblock = queries.reshape(nblk, WINDOW, kheads, group, HEAD).astype(jnp.float32)

    def band(arr):
        first = arr[:rows].reshape(nblk, WINDOW, kheads, HEAD)
        second = arr[WINDOW:].reshape(nblk, WINDOW, kheads, HEAD)
        return jnp.concatenate([first, second], axis=1).astype(jnp.float32)

    kband = band(keys_ext)
    vband = band(values_ext)
    score = jnp.einsum("nqhgd,nkhd->nhgqk", qblock, kband) * HEAD ** (-0.5)
    qidx = jnp.arange(WINDOW)[:, None]
    kidx = jnp.arange(2 * WINDOW)[None, :]
    rel = qidx + WINDOW - kidx
    valid = (rel >= 0) & (rel < WINDOW)
    blocks = block_base + jnp.arange(nblk)
    valid = valid[None] & ((blocks > 0)[:, None, None] | (kidx >= WINDOW)[None])
    score = jnp.where(valid[:, None, None], score, -jnp.inf)
    sink = sinks.reshape(kheads, group)[None, :, :, None]
    top = jnp.maximum(jnp.max(score, axis=-1), sink)
    expd = jnp.exp(score - top[..., None])
    denom = jnp.sum(expd, axis=-1) + jnp.exp(sink - top)
    weights = (expd / denom[..., None]).astype(jnp.bfloat16)
    result = jnp.einsum("nhgqk,nkhd->nqhgd", weights.astype(jnp.float32), vband)
    return result.reshape(rows, qheads * HEAD).astype(jnp.bfloat16)


def ring_order(count):
    return list(range(0, count, 2)) + list(range(1, count, 2))[::-1]


def uses_ring(count, widths):
    return count > 1 and count % 2 == 0 and min(widths) >= LANES


def ring_hops(shard, axis, dim):
    count = lax.axis_size(axis)
    if not uses_ring(count, (shard.shape[dim],)):
        return [[(jnp.uint32(0), lax.all_gather(shard, axis, axis=dim, tiled=True))]]
    order = ring_order(count)
    place = [0] * count
    for at, dev in enumerate(order):
        place[dev] = at
    table = [[order[(place[dev] + step) % count] for step in range(count)] for dev in range(count)]
    owners = jnp.array(table, jnp.uint32)[lax.axis_index(axis)]
    ahead = [(order[i], order[(i + 1) % count]) for i in range(count)]
    back = [(dst, src) for src, dst in ahead]

    def owner(step):
        return owners[step % count]

    hops = [[(owner(0), shard)]]
    from_left = from_right = shard
    for step in range(1, count // 2):
        from_left = lax.ppermute(from_left, axis, ahead)
        from_right = lax.ppermute(from_right, axis, back)
        hops.append([(owner(-step), from_left), (owner(step), from_right)])
    half = shard.shape[0] // 2
    top = lax.ppermute(from_left[:half], axis, ahead)
    bottom = lax.ppermute(from_right[half:], axis, back)
    hops.append([(owner(count // 2), jnp.concatenate([top, bottom], axis=0))])
    return hops


def shards(
    residual,
    queries,
    keys,
    values,
    sinks,
    out_weight,
    norm_gain,
    gate_weight,
    up_weight,
    down_weight,
):
    rows_dev = queries.shape[0]
    prev_keys, prev_values = passed_along((keys[-WINDOW:], values[-WINDOW:]), "sp", 1)
    gate_hops = ring_hops(gate_weight, "sp", 0)
    up_hops = ring_hops(up_weight, "sp", 0)
    down_hops = ring_hops(down_weight, "sp", 1)

    keys_ext = jnp.concatenate([prev_keys, keys], axis=0)
    values_ext = jnp.concatenate([prev_values, values], axis=0)
    attention = attend(
        queries, keys_ext, values_ext, sinks, lax.axis_index("sp") * (rows_dev // WINDOW)
    )
    attention = lax.all_to_all(attention, "tp", split_axis=0, concat_axis=1, tiled=True)
    proj = jnp.dot(attention, out_weight, preferred_element_type=jnp.float32)
    mixed = (residual.astype(jnp.float32) + proj).astype(jnp.bfloat16)
    mixf = mixed.astype(jnp.float32)
    normed = (
        mixf * lax.rsqrt(jnp.mean(mixf * mixf, axis=-1, keepdims=True) + 1e-06) * norm_gain
    ).astype(jnp.bfloat16)
    normed_all = lax.all_gather(normed, "tp", axis=0, tiled=True)

    def contracted(hops):
        total = None
        for hop in hops:
            for owner, block in hop:
                depth = block.shape[0]
                rows = lax.dynamic_slice_in_dim(normed_all, owner * depth, depth, 1)
                part = jnp.dot(rows, block, preferred_element_type=jnp.float32)
                total = part if total is None else total + part
        return total

    gate = contracted(gate_hops)
    upper = contracted(up_hops)
    hidden = (jax.nn.silu(gate) * upper).astype(jnp.bfloat16)
    groups = down_hops[1:]
    groups = [down_hops[0] + groups[0]] + groups[1:] if groups else down_hops
    out = mixed
    for group in groups:
        parts = [
            jnp.dot(hidden, block, preferred_element_type=jnp.float32).astype(jnp.bfloat16)
            for _, block in group
        ]
        terms = jnp.concatenate(parts, axis=1)
        ffn = lax.psum_scatter(terms, "tp", scatter_dimension=0, tiled=True).astype(jnp.float32)
        for at, (owner, block) in enumerate(group):
            width = block.shape[1]
            base = lax.dynamic_slice_in_dim(mixed, owner * width, width, 1).astype(jnp.float32)
            piece = (base + ffn[:, at * width : (at + 1) * width]).astype(jnp.bfloat16)
            out = lax.dynamic_update_slice_in_dim(out, piece, owner * width, 1)
    return out


def solution(mesh):
    placed = (
        P(("sp", "tp"), None),
        P("sp", "tp"),
        P("sp", "tp"),
        P("sp", "tp"),
        P("tp"),
        P(),
        P(),
        P("sp", "tp"),
        P("sp", "tp"),
        P("tp", "sp"),
    )
    return jax.shard_map(
        shards, mesh=mesh, in_specs=placed, out_specs=P(("sp", "tp"), None), check_vma=False
    )
```

```python
import jax
import jax.numpy as jnp
from jax import lax
from jax.experimental import pallas as pl
from jax.experimental.pallas import tpu as pltpu
from jax.sharding import PartitionSpec as P


HEAD = 64
WINDOW = 128
LANES = 128


def passed_along(block, axis, distance):
    devices = range(lax.axis_size(axis))
    route = [(i - distance, i) for i in devices if i - distance in devices]
    return lax.ppermute(block, axis, route)


def attend(queries, keys_ext, values_ext, sinks, block_base):
    rows = queries.shape[0]
    nblk = rows // WINDOW
    qheads = sinks.shape[0]
    kheads = keys_ext.shape[1] // HEAD
    group = qheads // kheads
    qblock = queries.reshape(nblk, WINDOW, kheads, group, HEAD).astype(jnp.float32)

    def band(arr):
        first = arr[:rows].reshape(nblk, WINDOW, kheads, HEAD)
        second = arr[WINDOW:].reshape(nblk, WINDOW, kheads, HEAD)
        return jnp.concatenate([first, second], axis=1).astype(jnp.float32)

    kband = band(keys_ext)
    vband = band(values_ext)
    score = jnp.einsum("nqhgd,nkhd->nhgqk", qblock, kband) * HEAD ** (-0.5)
    qidx = jnp.arange(WINDOW)[:, None]
    kidx = jnp.arange(2 * WINDOW)[None, :]
    rel = qidx + WINDOW - kidx
    valid = (rel >= 0) & (rel < WINDOW)
    blocks = block_base + jnp.arange(nblk)
    valid = valid[None] & ((blocks > 0)[:, None, None] | (kidx >= WINDOW)[None])
    score = jnp.where(valid[:, None, None], score, -jnp.inf)
    sink = sinks.reshape(kheads, group)[None, :, :, None]
    top = jnp.maximum(jnp.max(score, axis=-1), sink)
    expd = jnp.exp(score - top[..., None])
    denom = jnp.sum(expd, axis=-1) + jnp.exp(sink - top)
    weights = (expd / denom[..., None]).astype(jnp.bfloat16)
    result = jnp.einsum("nhgqk,nkhd->nqhgd", weights.astype(jnp.float32), vband)
    return result.reshape(rows, qheads * HEAD).astype(jnp.bfloat16)


def ring_order(count):
    return list(range(0, count, 2)) + list(range(1, count, 2))[::-1]


def widen_body(starts, normed, *refs):
    count = (len(refs) - 2) // 2
    gates, ups = refs[:count], refs[count : 2 * count]
    hidden, ordered = refs[-2:]
    base = 0
    for at, ref in enumerate(gates):
        depth = ref.shape[0]
        first = pl.multiple_of(starts[at], LANES)
        ordered[:, base : base + depth] = normed[:, pl.ds(first, depth)]
        base += depth
    total = hidden.shape[1]
    rows = ordered[...]
    for low in range(0, total, 2 * LANES):
        high = min(low + 2 * LANES, total)
        gate = jnp.dot(
            rows,
            jnp.concatenate([ref[:, low:high] for ref in gates], axis=0),
            preferred_element_type=jnp.float32,
        )
        upper = jnp.dot(
            rows,
            jnp.concatenate([ref[:, low:high] for ref in ups], axis=0),
            preferred_element_type=jnp.float32,
        )
        hidden[:, low:high] = (gate / (1.0 + jnp.exp(-gate)) * upper).astype(jnp.bfloat16)


def widened(normed, gates, ups, starts):
    rows, depth = normed.shape
    total = gates[0].shape[1]
    tile = 256 if rows % 256 == 0 else rows
    fixed = [pl.BlockSpec(block.shape, lambda i, s: (0, 0)) for block in gates + ups]
    return pl.pallas_call(
        widen_body,
        grid_spec=pltpu.PrefetchScalarGridSpec(
            num_scalar_prefetch=1,
            grid=(rows // tile,),
            in_specs=[pl.BlockSpec((tile, depth), lambda i, s: (i, 0))] + fixed,
            out_specs=pl.BlockSpec((tile, total), lambda i, s: (i, 0)),
            scratch_shapes=[pltpu.VMEM((tile, depth), jnp.bfloat16)],
        ),
        out_shape=jax.ShapeDtypeStruct((rows, total), jnp.bfloat16),
        compiler_params=pltpu.CompilerParams(
            dimension_semantics=("arbitrary",), vmem_limit_bytes=48 * 1024 * 1024
        ),
        cost_estimate=pl.CostEstimate(
            flops=4 * rows * depth * total,
            transcendentals=rows * total,
            bytes_accessed=4 * depth * total + 2 * rows * (depth + total),
        ),
    )(starts, normed, *gates, *ups)


def exchanged(blocks):
    count = lax.axis_size("tp")
    me = lax.axis_index("tp").astype(jnp.uint32)
    size = blocks.shape[0] // count
    pairs = []
    for step in range(count):
        there = (me + step) % count
        block = lax.dynamic_slice_in_dim(blocks, there * size, size, 0)
        if step:
            block = lax.ppermute(block, "tp", [(i, (i + step) % count) for i in range(count)])
        pairs.append(((me + count - step) % count, block))
    return pairs


def uses_ring(count, widths):
    return count > 1 and count % 2 == 0 and min(widths) >= LANES


def ring_hops(shard, axis, dim):
    count = lax.axis_size(axis)
    if not uses_ring(count, (shard.shape[dim],)):
        return [[(jnp.uint32(0), 0, lax.all_gather(shard, axis, axis=dim, tiled=True))]]
    order = ring_order(count)
    place = [0] * count
    for at, dev in enumerate(order):
        place[dev] = at
    table = [[order[(place[dev] + step) % count] for step in range(count)] for dev in range(count)]
    owners = jnp.array(table, jnp.uint32)[lax.axis_index(axis)]
    ahead = [(order[i], order[(i + 1) % count]) for i in range(count)]
    back = [(dst, src) for src, dst in ahead]

    def owner(step):
        return owners[step % count]

    hops = [[(owner(0), 0, shard)]]
    from_left = from_right = shard
    for step in range(1, count // 2):
        from_left = lax.ppermute(from_left, axis, ahead)
        from_right = lax.ppermute(from_right, axis, back)
        hops.append([(owner(-step), 0, from_left), (owner(step), 0, from_right)])
    half = shard.shape[0] // 2
    top = lax.ppermute(from_left[:half], axis, ahead)
    bottom = lax.ppermute(from_right[half:], axis, back)
    hops.append([(owner(count // 2), 0, top), (owner(count // 2), half, bottom)])
    return hops


def shards(
    residual,
    queries,
    keys,
    values,
    sinks,
    out_weight,
    norm_gain,
    gate_weight,
    up_weight,
    down_weight,
):
    rows_dev = queries.shape[0]
    prev_keys, prev_values = passed_along((keys[-WINDOW:], values[-WINDOW:]), "sp", 1)
    gate_hops = ring_hops(gate_weight, "sp", 0)
    up_hops = ring_hops(up_weight, "sp", 0)
    down_hops = ring_hops(down_weight, "sp", 1)

    keys_ext = jnp.concatenate([prev_keys, keys], axis=0)
    values_ext = jnp.concatenate([prev_values, values], axis=0)
    attention = attend(
        queries, keys_ext, values_ext, sinks, lax.axis_index("sp") * (rows_dev // WINDOW)
    )
    swapped = exchanged(attention)
    width = attention.shape[1]
    heads = jnp.zeros((residual.shape[0], out_weight.shape[0]), jnp.bfloat16)
    for source, block in swapped:
        heads = lax.dynamic_update_slice_in_dim(heads, block, source * width, 1)
    proj = jnp.dot(heads, out_weight, preferred_element_type=jnp.float32)
    mixed = (residual.astype(jnp.float32) + proj).astype(jnp.bfloat16)
    mixf = mixed.astype(jnp.float32)
    normed = (
        mixf * lax.rsqrt(jnp.mean(mixf * mixf, axis=-1, keepdims=True) + 1e-06) * norm_gain
    ).astype(jnp.bfloat16)
    normed_all = lax.all_gather(normed, "tp", axis=0, tiled=True)

    depth = gate_hops[0][0][2].shape[0]
    pieces = [piece for hop in gate_hops for piece in hop]
    starts = jnp.stack([owner.astype(jnp.int32) * depth + at for owner, at, _ in pieces])
    gates = [block for _, _, block in pieces]
    ups = [block for hop in up_hops for _, _, block in hop]
    hidden = widened(normed_all, gates, ups, starts)

    merged = [[(owner, block) for owner, _, block in hop] for hop in down_hops]
    if len(merged) > 1:
        merged[-1] = [
            (merged[-1][0][0], jnp.concatenate([block for _, block in merged[-1]], axis=0))
        ]
        merged = [merged[0] + merged[1]] + merged[2:]
    out = mixed
    for group in merged:
        parts = [
            jnp.dot(hidden, block, preferred_element_type=jnp.float32).astype(jnp.bfloat16)
            for _, block in group
        ]
        terms = jnp.concatenate(parts, axis=1)
        ffn = sum(block.astype(jnp.float32) for _, block in exchanged(terms))
        for at, (owner, block) in enumerate(group):
            width = block.shape[1]
            base = lax.dynamic_slice_in_dim(mixed, owner * width, width, 1).astype(jnp.float32)
            piece = (base + ffn[:, at * width : (at + 1) * width]).astype(jnp.bfloat16)
            out = lax.dynamic_update_slice_in_dim(out, piece, owner * width, 1)
    return out


def solution(mesh):
    placed = (
        P(("sp", "tp"), None),
        P("sp", "tp"),
        P("sp", "tp"),
        P("sp", "tp"),
        P("tp"),
        P(),
        P(),
        P("sp", "tp"),
        P("sp", "tp"),
        P("tp", "sp"),
    )
    return jax.shard_map(
        shards, mesh=mesh, in_specs=placed, out_specs=P(("sp", "tp"), None), check_vma=False
    )
```

```python
import functools

import jax
import jax.numpy as jnp
from jax import lax
from jax.experimental import pallas as pl
from jax.experimental.pallas import tpu as pltpu
from jax.sharding import PartitionSpec as P


HEAD = 64
WINDOW = 128
LANES = 128


def passed_along(block, axis, distance):
    devices = range(lax.axis_size(axis))
    route = [(i - distance, i) for i in devices if i - distance in devices]
    return lax.ppermute(block, axis, route)


def attend(queries, keys_ext, values_ext, sinks, block_base):
    rows = queries.shape[0]
    nblk = rows // WINDOW
    qheads = sinks.shape[0]
    kheads = keys_ext.shape[1] // HEAD
    group = qheads // kheads
    qblock = queries.reshape(nblk, WINDOW, kheads, group, HEAD).astype(jnp.float32)

    def band(arr):
        first = arr[:rows].reshape(nblk, WINDOW, kheads, HEAD)
        second = arr[WINDOW:].reshape(nblk, WINDOW, kheads, HEAD)
        return jnp.concatenate([first, second], axis=1).astype(jnp.float32)

    kband = band(keys_ext)
    vband = band(values_ext)
    score = jnp.einsum("nqhgd,nkhd->nhgqk", qblock, kband) * HEAD ** (-0.5)
    qidx = jnp.arange(WINDOW)[:, None]
    kidx = jnp.arange(2 * WINDOW)[None, :]
    rel = qidx + WINDOW - kidx
    valid = (rel >= 0) & (rel < WINDOW)
    blocks = block_base + jnp.arange(nblk)
    valid = valid[None] & ((blocks > 0)[:, None, None] | (kidx >= WINDOW)[None])
    score = jnp.where(valid[:, None, None], score, -jnp.inf)
    sink = sinks.reshape(kheads, group)[None, :, :, None]
    top = jnp.maximum(jnp.max(score, axis=-1), sink)
    expd = jnp.exp(score - top[..., None])
    denom = jnp.sum(expd, axis=-1) + jnp.exp(sink - top)
    weights = (expd / denom[..., None]).astype(jnp.bfloat16)
    result = jnp.einsum("nhgqk,nkhd->nqhgd", weights.astype(jnp.float32), vband)
    return result.reshape(rows, qheads * HEAD).astype(jnp.bfloat16)


def ring_order(count):
    return list(range(0, count, 2)) + list(range(1, count, 2))[::-1]


def widen_body(parts, starts, *refs):
    normed, refs = refs[:parts], refs[parts:]
    count = (len(refs) - 2) // 2
    gates, ups = refs[:count], refs[count : 2 * count]
    hidden, ordered = refs[-2:]
    base = 0
    for at, ref in enumerate(gates):
        depth = ref.shape[0]
        first = pl.multiple_of(starts[at], LANES)
        for part, block in enumerate(normed):
            size = block.shape[0]
            ordered[part * size : (part + 1) * size, base : base + depth] = block[
                :, pl.ds(first, depth)
            ]
        base += depth
    total = hidden.shape[1]
    rows = ordered[...]
    for low in range(0, total, 2 * LANES):
        high = min(low + 2 * LANES, total)
        gate = jnp.dot(
            rows,
            jnp.concatenate([ref[:, low:high] for ref in gates], axis=0),
            preferred_element_type=jnp.float32,
        )
        upper = jnp.dot(
            rows,
            jnp.concatenate([ref[:, low:high] for ref in ups], axis=0),
            preferred_element_type=jnp.float32,
        )
        hidden[:, low:high] = (gate / (1.0 + jnp.exp(-gate)) * upper).astype(jnp.bfloat16)


def widened(normed, gates, ups, starts):
    rows, depth = len(normed) * normed[0].shape[0], normed[0].shape[1]
    total = gates[0].shape[1]
    operands = [*normed, *gates, *ups]
    return pl.pallas_call(
        functools.partial(widen_body, len(normed)),
        grid_spec=pltpu.PrefetchScalarGridSpec(
            num_scalar_prefetch=1,
            grid=(1,),
            in_specs=[pl.BlockSpec(block.shape, lambda i, s: (0, 0)) for block in operands],
            out_specs=pl.BlockSpec((rows, total), lambda i, s: (0, 0)),
            scratch_shapes=[pltpu.VMEM((rows, depth), jnp.bfloat16)],
        ),
        out_shape=jax.ShapeDtypeStruct((rows, total), jnp.bfloat16),
        compiler_params=pltpu.CompilerParams(
            dimension_semantics=("arbitrary",), vmem_limit_bytes=48 * 1024 * 1024
        ),
        cost_estimate=pl.CostEstimate(
            flops=4 * rows * depth * total,
            transcendentals=rows * total,
            bytes_accessed=4 * depth * total + 2 * rows * (depth + total),
        ),
    )(starts, *operands)


def rotated(block, step):
    count = lax.axis_size("tp")
    if step == 0:
        return block
    return lax.ppermute(block, "tp", [(i, (i + step) % count) for i in range(count)])


def source(step):
    count = lax.axis_size("tp")
    return (lax.axis_index("tp").astype(jnp.uint32) + count - step) % count


def exchanged(blocks):
    count = lax.axis_size("tp")
    size = blocks.shape[0] // count
    pairs = []
    for step in range(count):
        block = lax.dynamic_slice_in_dim(blocks, source(count - step) * size, size, 0)
        pairs.append((source(step), rotated(block, step)))
    return pairs


def uses_ring(count, widths):
    return count > 1 and count % 2 == 0 and min(widths) >= LANES


def ring_table(count):
    order = ring_order(count)
    place = [order.index(dev) for dev in range(count)]
    return [[order[(place[dev] + step) % count] for step in range(count)] for dev in range(count)]


def piece_starts(axis, depth, pieces):
    count = lax.axis_size(axis)
    if pieces == 1:
        return jnp.zeros((1,), jnp.int32)
    steps = [0]
    for step in range(1, count // 2):
        steps += [-step, step]
    rows = [
        [around[step % count] * depth for step in steps]
        + [around[count // 2] * depth, around[count // 2] * depth + depth // 2]
        for around in ring_table(count)
    ]
    return jnp.array(rows, jnp.int32)[lax.axis_index(axis).astype(jnp.uint32)]


def ring_hops(shard, axis, dim):
    count = lax.axis_size(axis)
    if not uses_ring(count, (shard.shape[dim],)):
        return [[(jnp.uint32(0), 0, lax.all_gather(shard, axis, axis=dim, tiled=True))]]
    order = ring_order(count)
    table = ring_table(count)
    owners = jnp.array(table, jnp.uint32)[lax.axis_index(axis)]
    ahead = [(order[i], order[(i + 1) % count]) for i in range(count)]
    back = [(dst, src) for src, dst in ahead]

    def owner(step):
        return owners[step % count]

    hops = [[(owner(0), 0, shard)]]
    from_left = from_right = shard
    for step in range(1, count // 2):
        from_left = lax.ppermute(from_left, axis, ahead)
        from_right = lax.ppermute(from_right, axis, back)
        hops.append([(owner(-step), 0, from_left), (owner(step), 0, from_right)])
    half = shard.shape[0] // 2
    top = lax.ppermute(from_left[:half], axis, ahead)
    bottom = lax.ppermute(from_right[half:], axis, back)
    hops.append([(owner(count // 2), 0, top), (owner(count // 2), half, bottom)])
    return hops


def shards(
    residual,
    queries,
    keys,
    values,
    sinks,
    out_weight,
    norm_gain,
    gate_weight,
    up_weight,
    down_weight,
):
    rows_dev = queries.shape[0]
    prev_keys, prev_values = passed_along((keys[-WINDOW:], values[-WINDOW:]), "sp", 1)
    gate_hops = ring_hops(gate_weight, "sp", 0)
    up_hops = ring_hops(up_weight, "sp", 0)
    down_hops = ring_hops(down_weight, "sp", 1)

    keys_ext = jnp.concatenate([prev_keys, keys], axis=0)
    values_ext = jnp.concatenate([prev_values, values], axis=0)
    attention = attend(
        queries, keys_ext, values_ext, sinks, lax.axis_index("sp") * (rows_dev // WINDOW)
    )
    swapped = exchanged(attention)
    width = attention.shape[1]
    heads = jnp.zeros((residual.shape[0], out_weight.shape[0]), jnp.bfloat16)
    for source, block in swapped:
        heads = lax.dynamic_update_slice_in_dim(heads, block, source * width, 1)
    proj = jnp.dot(heads, out_weight, preferred_element_type=jnp.float32)
    mixed = (residual.astype(jnp.float32) + proj).astype(jnp.bfloat16)
    mixf = mixed.astype(jnp.float32)
    normed = (
        mixf * lax.rsqrt(jnp.mean(mixf * mixf, axis=-1, keepdims=True) + 1e-06) * norm_gain
    ).astype(jnp.bfloat16)
    peers = lax.axis_size("tp")
    normed_all = [rotated(normed, step) for step in range(peers)]

    depth = gate_hops[0][0][2].shape[0]
    pieces = [piece for hop in gate_hops for piece in hop]
    starts = piece_starts("sp", depth, len(pieces))
    gates = [block for _, _, block in pieces]
    ups = [block for hop in up_hops for _, _, block in hop]
    hidden = widened(normed_all, gates, ups, starts)

    merged = [[(owner, block) for owner, _, block in hop] for hop in down_hops]
    if len(merged) > 1:
        merged[-1] = [
            (merged[-1][0][0], jnp.concatenate([block for _, block in merged[-1]], axis=0))
        ]
        merged = [merged[0] + merged[1]] + merged[2:]
    out = mixed
    for group in merged:
        parts = [
            jnp.dot(hidden, block, preferred_element_type=jnp.float32).astype(jnp.bfloat16)
            for _, block in group
        ]
        terms = jnp.concatenate(parts, axis=1)
        size = terms.shape[0] // peers
        ffn = 0.0
        for step in range(peers):
            low = (peers - step) % peers * size
            block = rotated(terms[low : low + size], step)
            ffn = ffn + block.astype(jnp.float32)
        for at, (owner, block) in enumerate(group):
            width = block.shape[1]
            base = lax.dynamic_slice_in_dim(mixed, owner * width, width, 1).astype(jnp.float32)
            piece = (base + ffn[:, at * width : (at + 1) * width]).astype(jnp.bfloat16)
            out = lax.dynamic_update_slice_in_dim(out, piece, owner * width, 1)
    return out


def solution(mesh):
    placed = (
        P(("sp", "tp"), None),
        P("sp", "tp"),
        P("sp", "tp"),
        P("sp", "tp"),
        P("tp"),
        P(),
        P(),
        P("sp", "tp"),
        P("sp", "tp"),
        P("tp", "sp"),
    )
    return jax.shard_map(
        shards, mesh=mesh, in_specs=placed, out_specs=P(("sp", "tp"), None), check_vma=False
    )
```
